512 devices in a mesh: sp: 128 (over z, x, core), tp: 4 (over y).
Axes of the slice: x: 4, y: 4, z: 16, core: 2. Of those that a mesh axis runs over, the one named last changes fastest.
Arguments:
- conv_gate: bfloat16 [32768, 512], P('sp', 'tp'), may hold values from -6 to 6
- conv_mix: bfloat16 [32768, 512], P('sp', 'tp'), may hold values from -6 to 6
- conv_input: bfloat16 [32768, 512], P('sp', 'tp'), may hold values from -6 to 6
- conv_taps: bfloat16 [3, 512], P(None, 'tp'), may hold values from -3.5 to 3.5
- query_rows: bfloat16 [32768, 512], P('sp', 'tp'), may hold values from -50 to 50, as said below
- key_rows: bfloat16 [32768, 512], P('sp', 'tp'), may hold values from -10 to 10, as said below
- value_rows: bfloat16 [32768, 512], P('sp', 'tp'), may hold values from -6 to 6
- lambdas: float32 [4], P('tp'), may hold values from 0.3 to 0.8
- head_gain: float32 [128], replicated, may hold values from 0.1 to 1.9
- w_out_conv: bfloat16 [512, 2048], P('tp'), may hold values from -0.1875 to 0.1875
- w_out_heads: bfloat16 [512, 2048], P('tp'), may hold values from -0.1875 to 0.1875
Outputs:
- mixed: bfloat16 [32768, 2048], P(('sp', 'tp'))
The draws below stay inside these ranges and needn't reach their ends.
Inputs may be any that keep to these rules, and one draw needn't show every extreme that they name: `query_rows`: queries of order one; some rows may be far larger. `key_rows`: keys of order one.
All inputs are finite; a program needn't handle non-finite values.
Results may differ from the reference program's by a relative error of at most 0.013.
Values may be sent and summed in bfloat16 or wider, within the bound.
No kernel may reach another device: no remote copies, remote signals or barrier semaphores. Data moves between devices by JAX's collectives and lax.ppermute only.
A program may use at most 128 MiB of HBM per device.

```python
import math
import jax
import jax.numpy as jnp
from jax import lax

D = 2048
CONV = 512
QHEADS = 4
KVHEADS = 4
HEAD_QK = 64
HEAD_V = 128
TAPS = 3
TOKENS = 32768
N_TP = 4


def drawn_pair(key):
    base_key = jax.random.fold_in(key, 7)
    key_draw = jax.random.fold_in(base_key, 1)
    query_draw = jax.random.fold_in(base_key, 2)
    key_vals = jnp.clip(1.3 * jax.random.normal(key_draw, (TOKENS, KVHEADS, 2, HEAD_QK), jnp.float32), -8.0, 8.0)
    query_vals = jnp.clip(1.3 * jax.random.normal(query_draw, (TOKENS, QHEADS, 2, HEAD_QK), jnp.float32), -8.0, 8.0)
    return (query_vals.reshape(TOKENS, QHEADS * 2 * HEAD_QK), key_vals.reshape(TOKENS, KVHEADS * 2 * HEAD_QK))


def draw_query_rows(key, part):
    return drawn_pair(key)[0].astype(jnp.bfloat16)


def draw_key_rows(key, part):
    return drawn_pair(key)[1].astype(jnp.bfloat16)


def block_levels(own_key, dims, shards, least, high):
    factor_of, own = 1.0, jax.random.fold_in(own_key, 6)
    for position, shards_of in shards:
        draws = jnp.exp(jax.random.uniform(jax.random.fold_in(own, position), (shards_of,), jnp.float32, least / len(shards), high / len(shards)))
        factor_of = factor_of * jnp.repeat(draws, dims[position] // shards_of).reshape([-1 if axis == position else 1 for axis in range(len(dims))])
    return factor_of


def centred(rng, extent, scale, limit, shards=(), kind=jnp.bfloat16):
    entries = jax.random.normal(rng, extent, jnp.float32) * scale
    if len(shards) > 0:
        entries = block_levels(rng, extent, shards, -0.22, 0.18) * entries
    return jnp.clip(entries, min=-limit, max=limit).astype(kind)


def setup_inputs(seed: int = 0) -> dict:
    seeds = jax.random.split(jax.random.key(seed), 12)
    conv_gate = centred(seeds[0], (TOKENS, CONV), 1.0, 6.0, ((0, 128), (1, 4)))
    conv_mix = centred(seeds[1], (TOKENS, CONV), 1.0, 6.0, ((0, 128), (1, 4)))
    conv_input = centred(seeds[2], (TOKENS, CONV), 1.0, 6.0, ((0, 128), (1, 4)))
    conv_taps = centred(seeds[3], (TAPS, CONV), TAPS ** -0.5, 3.5, ((1, 4),))
    query_rows = draw_query_rows(jax.random.fold_in(seeds[11], 71), 0)
    key_rows = draw_key_rows(jax.random.fold_in(seeds[11], 71), 0)
    value_rows = centred(seeds[6], (TOKENS, KVHEADS * HEAD_V), 1.0, 6.0, ((0, 128), (1, 4)))
    lambdas = jnp.clip(0.3 + 0.5 * jax.random.uniform(seeds[7], (QHEADS,), jnp.float32) ** block_levels(seeds[7], (QHEADS,), ((0, 4),), -0.2, 0.2), 0.3, 0.8)
    head_gain = jnp.clip(1.0 + 0.18 * jax.random.normal(seeds[8], (HEAD_V,), jnp.float32), 0.1, 1.9)
    w_out_conv = centred(seeds[9], (CONV, D), (CONV + QHEADS * HEAD_V) ** -0.5, 0.1875, ((0, 4),))
    w_out_heads = centred(seeds[10], (QHEADS * HEAD_V, D), (CONV + QHEADS * HEAD_V) ** -0.5, 0.1875, ((0, 4),))
    return {"conv_gate": conv_gate, "conv_mix": conv_mix, "conv_input": conv_input, "conv_taps": conv_taps, "query_rows": query_rows, "key_rows": key_rows, "value_rows": value_rows, "lambdas": lambdas, "head_gain": head_gain, "w_out_conv": w_out_conv, "w_out_heads": w_out_heads}


def conv_branch(conv_gate, conv_mix, conv_input, conv_taps):
    gated_in = (conv_mix.astype(jnp.float32) * conv_input.astype(jnp.float32)).astype(jnp.bfloat16)
    padded = jnp.pad(gated_in, ((2, 0), (0, 0))).astype(jnp.float32)
    tap_values = conv_taps.astype(jnp.float32)
    convolved = tap_values[0] * padded[:-2] + tap_values[1] * padded[1:-1] + tap_values[2] * padded[2:]
    return (conv_gate.astype(jnp.float32) * convolved).astype(jnp.bfloat16)

def attention(query_rows, key_rows, value_rows, lambdas, head_gain):
    tokens = query_rows.shape[0]
    qblock = math.gcd(tokens, 256)
    group_size = QHEADS // KVHEADS
    scale_qk = HEAD_QK ** (-0.5)
    query_heads = query_rows.reshape(tokens, QHEADS, 2, HEAD_QK).astype(jnp.float32)
    key_heads = key_rows.reshape(tokens, KVHEADS, 2, HEAD_QK).astype(jnp.float32)
    value_heads = value_rows.reshape(tokens, KVHEADS, HEAD_V).astype(jnp.float32)
    key_positions = jnp.arange(tokens, dtype=jnp.int32)

    def one_block(block_index):
        offset_at = block_index * qblock
        query_block = lax.dynamic_slice_in_dim(query_heads, offset_at, qblock, 0)
        allowed = key_positions[None, :] <= (offset_at + jnp.arange(qblock, dtype=jnp.int32))[:, None]
        pieces = []
        for kv_head in range(KVHEADS):
            query_group = query_block[:, kv_head * group_size:(kv_head + 1) * group_size]
            scores = jnp.einsum('bhmd,tmd->hmbt', query_group, key_heads[:, kv_head]) * scale_qk
            scores = jnp.where(allowed, scores, -jnp.inf)
            peak_val = lax.optimization_barrier(jnp.max(scores, axis=-1, keepdims=True))
            weights = jnp.exp(scores - peak_val)
            denoms = lax.optimization_barrier(jnp.sum(weights, axis=-1))
            rounded = lax.optimization_barrier(weights.astype(jnp.bfloat16)).astype(jnp.float32)
            numerator = jnp.einsum('hmbt,te->hmbe', rounded, value_heads[:, kv_head])
            lambda_col = lambdas[kv_head * group_size:(kv_head + 1) * group_size][:, None, None]
            pieces.append(numerator[:, 0] / denoms[:, 0, :, None] - lambda_col * numerator[:, 1] / denoms[:, 1, :, None])
        merged = jnp.concatenate(pieces, axis=0)
        merged = merged * lax.rsqrt(lax.optimization_barrier(jnp.mean(merged * merged, axis=-1, keepdims=True)) + 1e-06) * head_gain * 0.8
        return jnp.transpose(merged, (1, 0, 2)).reshape(qblock, QHEADS * HEAD_V).astype(jnp.bfloat16)
    blocks_out = lax.map(one_block, jnp.arange(tokens // qblock, dtype=jnp.int32))
    return blocks_out.reshape(tokens, QHEADS * HEAD_V)

def reference(conv_gate, conv_mix, conv_input, conv_taps, query_rows, key_rows, value_rows, lambdas, head_gain, w_out_conv, w_out_heads):
    conv_out = conv_branch(conv_gate, conv_mix, conv_input, conv_taps)
    head_out = attention(query_rows, key_rows, value_rows, lambdas, head_gain)
    conv_width = CONV // N_TP
    head_width = QHEADS * HEAD_V // N_TP
    summed = jnp.zeros((conv_out.shape[0], D), jnp.float32)
    for group_index in range(N_TP):
        conv_part = jnp.dot(conv_out[:, group_index * conv_width:(group_index + 1) * conv_width], w_out_conv[group_index * conv_width:(group_index + 1) * conv_width], preferred_element_type=jnp.float32)
        head_part = jnp.dot(head_out[:, group_index * head_width:(group_index + 1) * head_width], w_out_heads[group_index * head_width:(group_index + 1) * head_width], preferred_element_type=jnp.float32)
        partial_value = (conv_part + head_part).astype(jnp.bfloat16)
        summed = summed + partial_value.astype(jnp.float32)
    return summed.astype(jnp.bfloat16)
```

```python
import math

import jax
import jax.numpy as jnp
from jax import lax
from jax.experimental import pallas as pl
from jax.experimental.pallas import tpu as pltpu
from jax.sharding import PartitionSpec as P

f32, bf16 = jnp.float32, jnp.bfloat16
HEAD_QK = 64
HEAD_V = 128
MAPS = 2
PLANES = 16
Q_STEP = 512
EARLY = 112
SCALE = HEAD_QK**-0.5 * math.log2(math.e)
LOW = -1e30
MASKED = -2e30
STAT = 16
OUT_ROWS = MAPS * (HEAD_V + STAT)
NN = (((1,), (0,)), ((), ()))


def flash_kernel(rows, first_row, resumed, last, at, q_ref, kv_ref, *refs):
    if resumed:
        m_in, acc_in, *refs = refs
    if last:
        out_ref, m_s, acc, qt, s_a, s_b, b_a, b_b = refs
    else:
        m_s, acc, qt, s_a, s_b, b_a, b_b = refs
    keys = kv_ref.shape[1]
    shards = q_ref.shape[0] // rows
    blocks = q_ref.shape[0] // Q_STEP
    z, j = at[0], at[1]

    def prepare(i, _):
        blk = q_ref[pl.ds(i * rows, rows), :].astype(f32).T * SCALE
        high = blk.astype(bf16).astype(f32)
        rest = blk - high
        for m in range(MAPS):
            lo, hi = HEAD_QK * m, HEAD_QK * (m + 1)
            qt[m, :, pl.ds(i * rows, rows)] = jnp.zeros((4 * HEAD_QK, rows), bf16)
            qt[m, lo:hi, pl.ds(i * rows, rows)] = high[lo:hi].astype(bf16)
            qt[m, 128 + lo : 128 + hi, pl.ds(i * rows, rows)] = rest[lo:hi].astype(bf16)
        return 0

    lax.fori_loop(0, shards, prepare, 0)
    if resumed:
        m_s[...] = m_in[...]
        acc[...] = acc_in[...]
    else:
        m_s[...] = jnp.full(m_s.shape, LOW, f32)
        acc[...] = jnp.zeros(acc.shape, f32)
    scores = ((s_a, b_a), (s_b, b_b))
    ahead = lax.broadcasted_iota(jnp.int32, (keys, rows), 0) - lax.broadcasted_iota(
        jnp.int32, (keys, rows), 1
    )

    def cols(b):
        return slice(b * Q_STEP, (b + 1) * Q_STEP)

    def score(i, b, diagonal):
        s_ref, b_ref = scores[b % 2]
        k = kv_ref[i, :, :128]
        k = jnp.concatenate([k, k], axis=1)
        for m in range(MAPS):
            s = lax.dot_general(k, qt[m, :, cols(b)], NN, preferred_element_type=f32)
            if diagonal:
                parts = []
                for h in range(Q_STEP // rows):
                    to = (b * (Q_STEP // rows) + h - j) * rows - first_row
                    parts.append(jnp.where(ahead <= to, s[:, h * rows : (h + 1) * rows], MASKED))
                s = jnp.concatenate(parts, axis=1)
            s_ref[m] = s
            b_ref[m] = jnp.max(s.reshape(keys // 8, 8, Q_STEP), axis=0)

    def weigh(v, b):
        s_ref, b_ref = scores[b % 2]
        for m in range(MAPS):
            old = m_s[m, :, cols(b)]
            new = jnp.maximum(old, jnp.max(b_ref[m], axis=0, keepdims=True))
            p = jnp.exp2(s_ref[m] - new[:1]).astype(bf16)
            shrink = jnp.exp2(old - new)
            m_s[m, :, cols(b)] = new
            o = lax.dot_general(v, p, NN, preferred_element_type=f32)
            acc[m, :, cols(b)] = acc[m, :, cols(b)] * shrink[:1] + o

    def values(i):
        v = kv_ref[i, :, 128:].astype(f32).T.astype(bf16)
        return jnp.concatenate([v, jnp.ones((STAT, keys), bf16)], axis=0)

    score(0, 0, False)

    def body(i, _):
        v = values(i)
        for b in range(blocks):
            if b + 1 < blocks:
                score(i, b + 1, False)
            else:
                score(i + 1, 0, False)
            weigh(v, b)
        return 0

    lax.fori_loop(0, z, body, 0)
    v = values(z)
    score(z, 0, True)
    for b in range(blocks):
        if b + 1 < blocks:
            score(z, b + 1, True)
        weigh(v, b)
    if not last:
        return

    def finish(s, _):
        for m in range(MAPS):
            a = acc[m, :, pl.ds(s * rows, rows)]
            den = jnp.maximum(a[HEAD_V : HEAD_V + 8], 1e-30)
            out_ref[s, HEAD_V * m : HEAD_V * (m + 1), :] = (a[:HEAD_V] * (1.0 / den[:1])).astype(
                bf16
            )
            rest = m_s[m, :, pl.ds(s * rows, rows)] + jnp.log2(den)
            parts = []
            for _part in range(3):
                hi = rest.astype(bf16).astype(f32)
                parts.append(hi)
                rest = rest - hi
            r = lax.broadcasted_iota(jnp.int32, rest.shape, 0)
            stat = jnp.where(r == 0, parts[0], jnp.where(r == 1, parts[1], parts[2]))
            at_row = MAPS * HEAD_V + STAT * m
            out_ref[s, at_row : at_row + STAT, :] = jnp.concatenate([stat, stat], axis=0).astype(
                bf16
            )
        return 0

    lax.fori_loop(0, shards, finish, 0)


def flash(at, q, kv, rows, first_row, state, last):
    queries = q.shape[0]
    keys = kv.shape[1]
    shapes = [(MAPS, 8, queries), (MAPS, HEAD_V + STAT, queries)]
    vmem = pl.BlockSpec(memory_space=pltpu.VMEM)
    scratch = [
        pltpu.VMEM((MAPS, 4 * HEAD_QK, queries), bf16),
        pltpu.VMEM((MAPS, keys, Q_STEP), f32),
        pltpu.VMEM((MAPS, keys, Q_STEP), f32),
        pltpu.VMEM((MAPS, 8, Q_STEP), f32),
        pltpu.VMEM((MAPS, 8, Q_STEP), f32),
    ]
    if last:
        out = jax.ShapeDtypeStruct((queries // rows, OUT_ROWS, rows), bf16)
        scratch = [pltpu.VMEM(s, f32) for s in shapes] + scratch
    else:
        out = [jax.ShapeDtypeStruct(s, f32) for s in shapes]

    def body(*refs):
        flash_kernel(rows, first_row, bool(state), last, *refs)

    return pl.pallas_call(
        body,
        out_shape=out,
        in_specs=[pl.BlockSpec(memory_space=pltpu.SMEM)] + [vmem] * (2 + len(state)),
        out_specs=vmem if last else [vmem, vmem],
        scratch_shapes=scratch,
        name="flash_last" if last else "flash_first",
    )(at, q, kv, *state)


def merge_kernel(lam, parts, gain, conv, w_conv, w_heads, out_ref):
    count, _, rows = parts.shape
    means = []
    for m in range(MAPS):
        at_row = MAPS * HEAD_V + STAT * m
        logs = []
        for d in range(count):
            stat = parts[d, at_row : at_row + STAT, :].astype(f32)
            logs.append(stat[0:1] + stat[1:2] + stat[2:3])
        peak = logs[0]
        for d in range(1, count):
            peak = jnp.maximum(peak, logs[d])
        weights = [jnp.exp2(x - peak) for x in logs]
        inverse = 1.0 / sum(weights)
        total = jnp.zeros((HEAD_V, rows), f32)
        for d in range(count):
            total += parts[d, HEAD_V * m : HEAD_V * (m + 1), :].astype(f32) * (
                weights[d] * inverse
            )
        means.append(total)
    diff = means[0] - lam[0] * means[1]
    square = jnp.mean(diff * diff, axis=0, keepdims=True)
    heads = (diff * lax.rsqrt(square + 1e-6)).T * (gain[...] * 0.8)
    out_ref[...] = (
        lax.dot_general(conv[...], w_conv[...], NN, preferred_element_type=f32)
        + lax.dot_general(heads.astype(bf16), w_heads[...], NN, preferred_element_type=f32)
    ).astype(bf16)


def merge(lambdas, parts, head_gain, conv_out, w_conv, w_heads):
    vmem = pl.BlockSpec(memory_space=pltpu.VMEM)
    return pl.pallas_call(
        merge_kernel,
        out_shape=jax.ShapeDtypeStruct((conv_out.shape[0], w_conv.shape[1]), bf16),
        in_specs=[pl.BlockSpec(memory_space=pltpu.SMEM)] + [vmem] * 5,
        out_specs=vmem,
        name="merge",
    )(lambdas, parts, head_gain[None, :], conv_out, w_conv, w_heads)


def conv_branch(conv_gate, conv_mix, conv_input, conv_taps):
    count = lax.axis_size("sp")
    gated_in = (conv_mix.astype(f32) * conv_input.astype(f32)).astype(bf16)
    before = lax.ppermute(gated_in[-2:], "sp", [(s, s + 1) for s in range(count - 1)])
    extended = jnp.concatenate([before, gated_in], axis=0).astype(f32)
    taps = conv_taps.astype(f32)
    convolved = taps[0] * extended[:-2] + taps[1] * extended[1:-1] + taps[2] * extended[2:]
    return (conv_gate.astype(f32) * convolved).astype(bf16)


def shards(
    conv_gate,
    conv_mix,
    conv_input,
    conv_taps,
    query_rows,
    key_rows,
    value_rows,
    lambdas,
    head_gain,
    w_out_conv,
    w_out_heads,
):
    rows = query_rows.shape[0]
    count = lax.axis_size("sp")
    in_plane = count // PLANES
    own = lax.axis_index("sp")
    at = jnp.stack([own // in_plane, own % in_plane]).astype(jnp.int32)
    plane = [[z * in_plane + j for j in range(in_plane)] for z in range(PLANES)]
    column = [[z * in_plane + j for z in range(PLANES)] for j in range(in_plane)]
    kv = jnp.concatenate([key_rows, value_rows], axis=1)
    late = lax.all_gather(kv[EARLY:], "sp", axis_index_groups=column)
    queries = lax.all_gather(query_rows, "sp", axis=0, tiled=True, axis_index_groups=plane)
    early = lax.all_gather(kv[:EARLY], "sp", axis_index_groups=column)
    conv_out = conv_branch(conv_gate, conv_mix, conv_input, conv_taps)
    state = flash(at, queries, early, rows, 0, (), False)
    partial_heads = flash(at, queries, late, rows, EARLY, tuple(state), True)
    arrived = lax.all_to_all(
        partial_heads, "sp", split_axis=0, concat_axis=0, tiled=True, axis_index_groups=plane
    )
    partial = merge(lambdas, arrived, head_gain, conv_out, w_out_conv, w_out_heads)
    ways = lax.axis_size("tp")
    pieces = lax.all_to_all(
        partial.reshape(ways, rows // ways, -1), "tp", split_axis=0, concat_axis=0, tiled=True
    )
    return pieces.astype(f32).sum(axis=0).astype(bf16)


def solution(mesh):
    placed = (
        P("sp", "tp"),
        P("sp", "tp"),
        P("sp", "tp"),
        P(None, "tp"),
        P("sp", "tp"),
        P("sp", "tp"),
        P("sp", "tp"),
        P("tp"),
        P(),
        P("tp", None),
        P("tp", None),
    )
    return jax.shard_map(
        shards, mesh=mesh, in_specs=placed, out_specs=P(("sp", "tp"), None), check_vma=False
    )
```

```python
import math

import jax
import jax.numpy as jnp
from jax import lax
from jax.experimental import pallas as pl
from jax.experimental.pallas import tpu as pltpu
from jax.sharding import PartitionSpec as P

f32, bf16 = jnp.float32, jnp.bfloat16
HEAD_QK = 64
HEAD_V = 128
MAPS = 2
PLANES = 16
CORES = 2
Q_STEP = 512
K_STEP = 256
EARLY = 112
SCALE = HEAD_QK**-0.5 * math.log2(math.e)
LOW = -1e30
MASKED = -2e30
STAT = 16
OUT_ROWS = MAPS * (HEAD_V + STAT)
NN = (((1,), (0,)), ((), ()))


def pack_kernel(q_ref, k_ref, v_ref, early_ref, late_ref, copies_ref):
    early_ref[:, :HEAD_V] = k_ref[:EARLY]
    early_ref[:, HEAD_V:] = v_ref[:EARLY]
    late_ref[:, :HEAD_V] = k_ref[EARLY:]
    late_ref[:, HEAD_V:] = v_ref[EARLY:]
    for i in range(copies_ref.shape[0]):
        copies_ref[i] = q_ref[...]


def pack(q, k, v, copies):
    rows, width = q.shape
    return pl.pallas_call(
        pack_kernel,
        out_shape=[
            jax.ShapeDtypeStruct((EARLY, 2 * width), bf16),
            jax.ShapeDtypeStruct((rows - EARLY, 2 * width), bf16),
            jax.ShapeDtypeStruct((copies, rows, width), bf16),
        ],
        name="pack",
    )(q, k, v)


def flash_kernel(rows, first_row, keys_each, last, at, q_ref, kv_ref, *refs):
    if last:
        m_hbm, acc_hbm, out_ref, m_s, acc, m_in, acc_in, sems, qt, s_a, s_b, b_a, b_b = refs
        copies = [
            pltpu.make_async_copy(m_hbm, m_in, sems.at[0]),
            pltpu.make_async_copy(acc_hbm, acc_in, sems.at[1]),
        ]
        for copy in copies:
            copy.start()
    else:
        m_s, acc, qt, s_a, s_b, b_a, b_b = refs
    shards = q_ref.shape[0] // rows
    blocks = q_ref.shape[0] // Q_STEP
    lines = shards // 2
    p, e, x, c = at[0], at[1], at[2], at[3]

    def prepare(i, _):
        blk = q_ref[pl.ds(i * rows, rows), :].astype(f32).T * SCALE
        high = blk.astype(bf16).astype(f32)
        rest = blk - high
        for m in range(MAPS):
            lo, hi = HEAD_QK * m, HEAD_QK * (m + 1)
            qt[m, :, pl.ds(i * rows, rows)] = jnp.zeros((4 * HEAD_QK, rows), bf16)
            qt[m, lo:hi, pl.ds(i * rows, rows)] = high[lo:hi].astype(bf16)
            qt[m, 128 + lo : 128 + hi, pl.ds(i * rows, rows)] = rest[lo:hi].astype(bf16)
        return 0

    lax.fori_loop(0, shards, prepare, 0)
    m_s[...] = jnp.full(m_s.shape, LOW, f32)
    acc[...] = jnp.zeros(acc.shape, f32)
    scores = ((s_a, b_a), (s_b, b_b))

    def cols(b):
        return slice(b * Q_STEP, (b + 1) * Q_STEP)

    def score(i, b, ahead):
        s_ref, b_ref = scores[b % 2]
        k = kv_ref[pl.ds(i * K_STEP, K_STEP), :HEAD_V]
        k = jnp.concatenate([k, k], axis=1)
        for m in range(MAPS):
            s = lax.dot_general(k, qt[m, :, cols(b)], NN, preferred_element_type=f32)
            if ahead is not None:
                parts = []
                for h in range(Q_STEP // rows):
                    g = b * (Q_STEP // rows) + h
                    first = ((g // lines) * shards + (g % lines) * CORES + c) * rows
                    parts.append(jnp.where(ahead <= first, s[:, h * rows : (h + 1) * rows], MASKED))
                s = jnp.concatenate(parts, axis=1)
            s_ref[m] = s
            b_ref[m] = jnp.max(s.reshape(K_STEP // 8, 8, Q_STEP), axis=0)

    def weigh(v, b):
        s_ref, b_ref = scores[b % 2]
        for m in range(MAPS):
            old = m_s[m, :, cols(b)]
            new = jnp.maximum(old, jnp.max(b_ref[m], axis=0, keepdims=True))
            weights = jnp.exp2(s_ref[m] - new[:1]).astype(bf16)
            shrink = jnp.exp2(old - new)
            m_s[m, :, cols(b)] = new
            o = lax.dot_general(v, weights, NN, preferred_element_type=f32)
            acc[m, :, cols(b)] = acc[m, :, cols(b)] * shrink[:1] + o

    def values(i):
        v = kv_ref[pl.ds(i * K_STEP, K_STEP), HEAD_V:].astype(f32).T.astype(bf16)
        return jnp.concatenate([v, jnp.ones((STAT, K_STEP), bf16)], axis=0)

    whole = CORES * p * keys_each
    full = whole // K_STEP
    end = (whole + CORES * keys_each + K_STEP - 1) // K_STEP
    score(0, 0, None)

    def body(i, _):
        v = values(i)
        for b in range(blocks):
            if b + 1 < blocks:
                score(i, b + 1, None)
            else:
                score(i + 1, 0, None)
            weigh(v, b)
        return 0

    lax.fori_loop(0, full, body, 0)

    def edge(i, _):
        n = lax.broadcasted_iota(jnp.int32, (K_STEP, rows), 0) + (i * K_STEP - whole)
        base = (e * shards + x * CORES) * rows + first_row
        place = jnp.where(n < keys_each, n + base, n + (base + rows - keys_each))
        place = jnp.where(n < 0, -rows, jnp.where(n < CORES * keys_each, place, 1 << 20))
        ahead = place - lax.broadcasted_iota(jnp.int32, (K_STEP, rows), 1)
        v = values(i)
        score(i, 0, ahead)
        for b in range(blocks):
            if b + 1 < blocks:
                score(i, b + 1, ahead)
            weigh(v, b)
        return 0

    lax.fori_loop(full, end, edge, 0)
    if not last:
        return
    for copy in copies:
        copy.wait()

    def finish(s, _):
        at_cols = pl.ds(s * rows, rows)
        for m in range(MAPS):
            peak = jnp.maximum(m_s[m, :, at_cols], m_in[m, :, at_cols])
            mine = jnp.exp2(m_s[m, :, at_cols] - peak)[:1]
            other = jnp.exp2(m_in[m, :, at_cols] - peak)[:1]
            a = acc[m, :, at_cols] * mine + acc_in[m, :, at_cols] * other
            den = jnp.maximum(a[HEAD_V : HEAD_V + 8], 1e-30)
            out_ref[s, HEAD_V * m : HEAD_V * (m + 1), :] = (a[:HEAD_V] * (1.0 / den[:1])).astype(
                bf16
            )
            rest = peak + jnp.log2(den)
            parts = []
            for _part in range(3):
                hi = rest.astype(bf16).astype(f32)
                parts.append(hi)
                rest = rest - hi
            r = lax.broadcasted_iota(jnp.int32, rest.shape, 0)
            stat = jnp.where(r == 0, parts[0], jnp.where(r == 1, parts[1], parts[2]))
            at_row = MAPS * HEAD_V + STAT * m
            out_ref[s, at_row : at_row + STAT, :] = jnp.concatenate([stat, stat], axis=0).astype(
                bf16
            )
        return 0

    lax.fori_loop(0, shards, finish, 0)


def flash(at, q, kv, rows, first_row, keys_each, state):
    queries = q.shape[0]
    shapes = [(MAPS, 8, queries), (MAPS, HEAD_V + STAT, queries)]
    vmem = pl.BlockSpec(memory_space=pltpu.VMEM)
    scratch = [
        pltpu.VMEM((MAPS, 4 * HEAD_QK, queries), bf16),
        pltpu.VMEM((MAPS, K_STEP, Q_STEP), f32),
        pltpu.VMEM((MAPS, K_STEP, Q_STEP), f32),
        pltpu.VMEM((MAPS, 8, Q_STEP), f32),
        pltpu.VMEM((MAPS, 8, Q_STEP), f32),
    ]
    last = bool(state)
    if last:
        out = jax.ShapeDtypeStruct((queries // rows, OUT_ROWS, rows), bf16)
        held = [pltpu.VMEM(s, f32) for s in shapes]
        scratch = held + held + [pltpu.SemaphoreType.DMA((2,))] + scratch
    else:
        out = [jax.ShapeDtypeStruct(s, f32) for s in shapes]

    def body(*refs):
        flash_kernel(rows, first_row, keys_each, last, *refs)

    return pl.pallas_call(
        body,
        out_shape=out,
        in_specs=[pl.BlockSpec(memory_space=pltpu.SMEM), vmem, vmem]
        + [pl.BlockSpec(memory_space=pl.ANY)] * len(state),
        out_specs=vmem if last else [vmem, vmem],
        scratch_shapes=scratch,
        name="flash_last" if last else "flash_first",
    )(at, q, kv, *state)


def merge_kernel(lam, parts, gain, conv, w_conv, w_heads, out_ref):
    count, _, rows = parts.shape
    means = []
    for m in range(MAPS):
        at_row = MAPS * HEAD_V + STAT * m
        logs = []
        for d in range(count):
            stat = parts[d, at_row : at_row + STAT, :].astype(f32)
            logs.append(stat[0:1] + stat[1:2] + stat[2:3])
        peak = logs[0]
        for d in range(1, count):
            peak = jnp.maximum(peak, logs[d])
        weights = [jnp.exp2(x - peak) for x in logs]
        inverse = 1.0 / sum(weights)
        total = jnp.zeros((HEAD_V, rows), f32)
        for d in range(count):
            total += parts[d, HEAD_V * m : HEAD_V * (m + 1), :].astype(f32) * (
                weights[d] * inverse
            )
        means.append(total)
    diff = means[0] - lam[0] * means[1]
    square = jnp.mean(diff * diff, axis=0, keepdims=True)
    heads = (diff * lax.rsqrt(square + 1e-6)).T * (gain[...] * 0.8)
    out_ref[...] = (
        lax.dot_general(conv[...], w_conv[...], NN, preferred_element_type=f32)
        + lax.dot_general(heads.astype(bf16), w_heads[...], NN, preferred_element_type=f32)
    ).astype(bf16)


def merge(lambdas, parts, head_gain, conv_out, w_conv, w_heads):
    vmem = pl.BlockSpec(memory_space=pltpu.VMEM)
    return pl.pallas_call(
        merge_kernel,
        out_shape=jax.ShapeDtypeStruct((conv_out.shape[0], w_conv.shape[1]), bf16),
        in_specs=[pl.BlockSpec(memory_space=pltpu.SMEM)] + [vmem] * 5,
        out_specs=vmem,
        name="merge",
    )(lambdas, parts, head_gain[None, :], conv_out, w_conv, w_heads)


def conv_branch(conv_gate, conv_mix, conv_input, conv_taps):
    count = lax.axis_size("sp")
    gated_in = (conv_mix.astype(f32) * conv_input.astype(f32)).astype(bf16)
    before = lax.ppermute(gated_in[-2:], "sp", [(s, s + 1) for s in range(count - 1)])
    extended = jnp.concatenate([before, gated_in], axis=0).astype(f32)
    taps = conv_taps.astype(f32)
    convolved = taps[0] * extended[:-2] + taps[1] * extended[1:-1] + taps[2] * extended[2:]
    return (conv_gate.astype(f32) * convolved).astype(bf16)


def shards(
    conv_gate,
    conv_mix,
    conv_input,
    conv_taps,
    query_rows,
    key_rows,
    value_rows,
    lambdas,
    head_gain,
    w_out_conv,
    w_out_heads,
):
    rows = query_rows.shape[0]
    count = lax.axis_size("sp")
    lines = count // (PLANES * CORES)
    own = lax.axis_index("sp")
    in_plane = lines * CORES
    z = own // in_plane
    at = jnp.stack([z // 2, z % 2, own % in_plane // CORES, own % CORES]).astype(jnp.int32)

    def place(p, e, x, c):
        return ((2 * p + e) * lines + x) * CORES + c

    peers = [
        [place(p, e, x, c) for e in range(2) for x in range(lines)]
        for p in range(PLANES // 2)
        for c in range(CORES)
    ]
    column = [
        [place(p, e, x, c) for p in range(PLANES // 2) for c in range(CORES)]
        for e in range(2)
        for x in range(lines)
    ]
    early, late, copies = pack(query_rows, key_rows, value_rows, 2 * lines)
    late = lax.all_gather(late, "sp", axis=0, tiled=True, axis_index_groups=column)
    queries = lax.all_to_all(
        copies, "sp", split_axis=0, concat_axis=0, tiled=True, axis_index_groups=peers
    ).reshape(2 * lines * rows, -1)
    early = lax.all_gather(early, "sp", axis=0, tiled=True, axis_index_groups=column)
    conv_out = conv_branch(conv_gate, conv_mix, conv_input, conv_taps)
    state = flash(at, queries, early, rows, 0, EARLY, ())
    partial_heads = flash(at, queries, late, rows, EARLY, rows - EARLY, tuple(state))
    arrived = lax.all_to_all(
        partial_heads, "sp", split_axis=0, concat_axis=0, tiled=True, axis_index_groups=peers
    )
    partial = merge(lambdas, arrived, head_gain, conv_out, w_out_conv, w_out_heads)
    ways = lax.axis_size("tp")
    pieces = lax.all_to_all(
        partial.reshape(ways, rows // ways, -1), "tp", split_axis=0, concat_axis=0, tiled=True
    )
    return pieces.astype(f32).sum(axis=0).astype(bf16)


def solution(mesh):
    placed = (
        P("sp", "tp"),
        P("sp", "tp"),
        P("sp", "tp"),
        P(None, "tp"),
        P("sp", "tp"),
        P("sp", "tp"),
        P("sp", "tp"),
        P("tp"),
        P(),
        P("tp", None),
        P("tp", None),
    )
    return jax.shard_map(
        shards, mesh=mesh, in_specs=placed, out_specs=P(("sp", "tp"), None), check_vma=False
    )
```

```python
import math

import jax
import jax.numpy as jnp
from jax import lax
from jax.experimental import pallas as pl
from jax.experimental.pallas import tpu as pltpu
from jax.sharding import PartitionSpec as P

f32, bf16 = jnp.float32, jnp.bfloat16
HEAD_QK = 64
HEAD_V = 128
MAPS = 2
PLANES = 16
CORES = 2
Q_STEP = 512
K_STEP = 256
EARLY = 112
SCALE = HEAD_QK**-0.5 * math.log2(math.e)
LOW = -1e30
MASKED = -2e30
STAT = 16
OUT_ROWS = HEAD_V + STAT
NN = (((1,), (0,)), ((), ()))


def pack_kernel(q_ref, k_ref, v_ref, early_ref, late_ref, copies_ref):
    early_ref[:, :HEAD_V] = k_ref[:EARLY]
    early_ref[:, HEAD_V:] = v_ref[:EARLY]
    late_ref[:, :HEAD_V] = k_ref[EARLY:]
    late_ref[:, HEAD_V:] = v_ref[EARLY:]
    for i in range(copies_ref.shape[0]):
        copies_ref[i] = q_ref[...]


def pack(q, k, v, copies):
    rows, width = q.shape
    return pl.pallas_call(
        pack_kernel,
        out_shape=[
            jax.ShapeDtypeStruct((EARLY, 2 * width), bf16),
            jax.ShapeDtypeStruct((rows - EARLY, 2 * width), bf16),
            jax.ShapeDtypeStruct((copies, rows, width), bf16),
        ],
        name="pack",
    )(q, k, v)


def flash_kernel(rows, first_row, keys_each, last, at, q_ref, kv_ref, *refs):
    if last:
        lam, m_hbm, acc_hbm, out_ref, m_s, acc, m_in, acc_in, sems, qt, s_a, s_b, b_a, b_b = refs
        copies = [
            pltpu.make_async_copy(m_hbm, m_in, sems.at[0]),
            pltpu.make_async_copy(acc_hbm, acc_in, sems.at[1]),
        ]
        for copy in copies:
            copy.start()
    else:
        m_s, acc, qt, s_a, s_b, b_a, b_b = refs
    shards = q_ref.shape[0] // rows
    blocks = q_ref.shape[0] // Q_STEP
    lines = shards // 2
    p, e, x, c = at[0], at[1], at[2], at[3]

    def prepare(i, _):
        blk = q_ref[pl.ds(i * rows, rows), :].astype(f32).T * SCALE
        high = blk.astype(bf16).astype(f32)
        rest = blk - high
        for m in range(MAPS):
            lo, hi = HEAD_QK * m, HEAD_QK * (m + 1)
            qt[m, :, pl.ds(i * rows, rows)] = jnp.zeros((4 * HEAD_QK, rows), bf16)
            qt[m, lo:hi, pl.ds(i * rows, rows)] = high[lo:hi].astype(bf16)
            qt[m, 128 + lo : 128 + hi, pl.ds(i * rows, rows)] = rest[lo:hi].astype(bf16)
        return 0

    lax.fori_loop(0, shards, prepare, 0)
    m_s[...] = jnp.full(m_s.shape, LOW, f32)
    acc[...] = jnp.zeros(acc.shape, f32)
    scores = ((s_a, b_a), (s_b, b_b))

    def cols(b):
        return slice(b * Q_STEP, (b + 1) * Q_STEP)

    def score(i, b, ahead):
        s_ref, b_ref = scores[b % 2]
        k = kv_ref[pl.ds(i * K_STEP, K_STEP), :HEAD_V]
        k = jnp.concatenate([k, k], axis=1)
        for m in range(MAPS):
            s = lax.dot_general(k, qt[m, :, cols(b)], NN, preferred_element_type=f32)
            if ahead is not None:
                parts = []
                for h in range(Q_STEP // rows):
                    g = b * (Q_STEP // rows) + h
                    first = ((g // lines) * shards + (g % lines) * CORES + c) * rows
                    parts.append(jnp.where(ahead <= first, s[:, h * rows : (h + 1) * rows], MASKED))
                s = jnp.concatenate(parts, axis=1)
            s_ref[m] = s
            b_ref[m] = jnp.max(s.reshape(K_STEP // 8, 8, Q_STEP), axis=0)

    def weigh(v, b):
        s_ref, b_ref = scores[b % 2]
        for m in range(MAPS):
            old = m_s[m, :, cols(b)]
            new = jnp.maximum(old, jnp.max(b_ref[m], axis=0, keepdims=True))
            weights = jnp.exp2(s_ref[m] - new[:1]).astype(bf16)
            shrink = jnp.exp2(old - new)
            m_s[m, :, cols(b)] = new
            o = lax.dot_general(v, weights, NN, preferred_element_type=f32)
            acc[m, :, cols(b)] = acc[m, :, cols(b)] * shrink[:1] + o

    def values(i):
        v = kv_ref[pl.ds(i * K_STEP, K_STEP), HEAD_V:].astype(f32).T.astype(bf16)
        return jnp.concatenate([v, jnp.ones((STAT, K_STEP), bf16)], axis=0)

    whole = CORES * p * keys_each
    full = whole // K_STEP
    end = (whole + CORES * keys_each + K_STEP - 1) // K_STEP
    score(0, 0, None)

    def body(i, _):
        v = values(i)
        for b in range(blocks):
            if b + 1 < blocks:
                score(i, b + 1, None)
            else:
                score(i + 1, 0, None)
            weigh(v, b)
        return 0

    lax.fori_loop(0, full, body, 0)

    def edge(i, _):
        n = lax.broadcasted_iota(jnp.int32, (K_STEP, rows), 0) + (i * K_STEP - whole)
        base = (e * shards + x * CORES) * rows + first_row
        place = jnp.where(n < keys_each, n + base, n + (base + rows - keys_each))
        place = jnp.where(n < 0, -rows, jnp.where(n < CORES * keys_each, place, 1 << 20))
        ahead = place - lax.broadcasted_iota(jnp.int32, (K_STEP, rows), 1)
        v = values(i)
        score(i, 0, ahead)
        for b in range(blocks):
            if b + 1 < blocks:
                score(i, b + 1, ahead)
            weigh(v, b)
        return 0

    lax.fori_loop(full, end, edge, 0)
    if not last:
        return
    for copy in copies:
        copy.wait()

    def finish(s, _):
        at_cols = pl.ds(s * rows, rows)
        sides = []
        for m in range(MAPS):
            peak = jnp.maximum(m_s[m, :, at_cols], m_in[m, :, at_cols])
            mine = jnp.exp2(m_s[m, :, at_cols] - peak)[:1]
            other = jnp.exp2(m_in[m, :, at_cols] - peak)[:1]
            a = acc[m, :, at_cols] * mine + acc_in[m, :, at_cols] * other
            den = jnp.maximum(a[HEAD_V : HEAD_V + 8], 1e-30)
            factor = lam[0] / den[:1] if m else 1.0 / den[:1]
            rest = peak + jnp.log2(den)
            parts = []
            for _part in range(3):
                hi = rest.astype(bf16).astype(f32)
                parts.append(hi)
                rest = rest - hi
            r = lax.broadcasted_iota(jnp.int32, rest.shape, 0)
            stat = jnp.where(r == 0, parts[0], jnp.where(r == 1, parts[1], parts[2]))
            sides.append(jnp.concatenate([a[:HEAD_V] * factor, stat, stat], axis=0))
        for t in range(rows // 128):
            first = sides[0][:, t * 128 : (t + 1) * 128]
            second = pltpu.roll(sides[1][:, t * 128 : (t + 1) * 128], 64, 1)
            lower = lax.broadcasted_iota(jnp.int32, first.shape, 1) < 64
            out_ref[s, 2 * t] = jnp.where(lower, first, second).astype(bf16)
            out_ref[s, 2 * t + 1] = jnp.where(lower, second, first).astype(bf16)
        return 0

    lax.fori_loop(0, shards, finish, 0)


def flash(at, q, kv, rows, first_row, keys_each, state):
    queries = q.shape[0]
    shapes = [(MAPS, 8, queries), (MAPS, HEAD_V + STAT, queries)]
    vmem = pl.BlockSpec(memory_space=pltpu.VMEM)
    scratch = [
        pltpu.VMEM((MAPS, 4 * HEAD_QK, queries), bf16),
        pltpu.VMEM((MAPS, K_STEP, Q_STEP), f32),
        pltpu.VMEM((MAPS, K_STEP, Q_STEP), f32),
        pltpu.VMEM((MAPS, 8, Q_STEP), f32),
        pltpu.VMEM((MAPS, 8, Q_STEP), f32),
    ]
    last = bool(state)
    if last:
        out = jax.ShapeDtypeStruct((queries // rows, rows // 64, OUT_ROWS, 128), bf16)
        held = [pltpu.VMEM(s, f32) for s in shapes]
        scratch = held + held + [pltpu.SemaphoreType.DMA((2,))] + scratch
    else:
        out = [jax.ShapeDtypeStruct(s, f32) for s in shapes]

    def body(*refs):
        flash_kernel(rows, first_row, keys_each, last, *refs)

    return pl.pallas_call(
        body,
        out_shape=out,
        in_specs=[pl.BlockSpec(memory_space=pltpu.SMEM), vmem, vmem]
        + [pl.BlockSpec(memory_space=pltpu.SMEM)] * (len(state) > 0)
        + [pl.BlockSpec(memory_space=pl.ANY)] * (len(state) - 1),
        out_specs=vmem if last else [vmem, vmem],
        scratch_shapes=scratch,
        name="flash_last" if last else "flash_first",
    )(at, q, kv, *state)


def merge_kernel(ways, tp, gain, *refs):
    sources, out_ref, held, sems = refs[: 2 + ways], refs[2 + ways], refs[3 + ways : -1], refs[-1]
    copies = [
        pltpu.make_async_copy(src, dst, sems.at[i])
        for i, (src, dst) in enumerate(zip(sources, held))
    ]
    parts, w, *conv = held
    for copy in copies:
        copy.start()
    copies[0].wait()
    count, _, _, lanes = parts.shape
    half = lanes // 2
    blocks = []
    for h in range(ways):
        logs = []
        for d in range(count):
            stat = parts[d, h, HEAD_V:, :].astype(f32)
            logs.append(stat[0:1] + stat[1:2] + stat[2:3])
        peak = logs[0]
        for d in range(1, count):
            peak = jnp.maximum(peak, logs[d])
        weights = [jnp.exp2(x - peak) for x in logs]
        inverse = 1.0 / sum(weights)
        total = jnp.zeros((HEAD_V, lanes), f32)
        for d in range(count):
            total += parts[d, h, :HEAD_V, :].astype(f32) * (weights[d] * inverse)
        diff = total - pltpu.roll(total, half, 1)
        square = jnp.mean(diff * diff, axis=0, keepdims=True)
        heads = (diff * lax.rsqrt(square + 1e-6)).T * (gain[...] * 0.8)
        blocks.append(jnp.where(tp[0] % 2 == 1, heads[half:], heads[:half]).astype(bf16))
    heads = jnp.concatenate(blocks, axis=1)
    copies[1].wait()
    mixed = lax.dot_general(heads, w[...], NN, preferred_element_type=f32)
    for i in range(ways):
        copies[2 + i].wait()
        mixed += conv[i][...].astype(f32)
    out_ref[...] = mixed.astype(bf16)


def merge(tp, head_gain, parts, w_heads, conv):
    out_rows, width = conv[0].shape
    ways = len(conv)

    def body(*refs):
        merge_kernel(ways, *refs)

    return pl.pallas_call(
        body,
        out_shape=jax.ShapeDtypeStruct((out_rows, width), bf16),
        in_specs=[pl.BlockSpec(memory_space=pltpu.SMEM), pl.BlockSpec(memory_space=pltpu.VMEM)]
        + [pl.BlockSpec(memory_space=pl.ANY)] * (2 + ways),
        out_specs=pl.BlockSpec(memory_space=pltpu.VMEM),
        scratch_shapes=[pltpu.VMEM(a.shape, bf16) for a in (parts, w_heads, *conv)]
        + [pltpu.SemaphoreType.DMA((2 + ways,))],
        name="merge",
    )(tp, head_gain[None, :], parts, w_heads, *conv)


def halo(conv_mix, conv_input):
    count = lax.axis_size("sp")
    gated_in = (conv_mix.astype(f32) * conv_input.astype(f32)).astype(bf16)
    return lax.ppermute(gated_in[-2:], "sp", [(s, s + 1) for s in range(count - 1)])


def conv_branch(before, conv_gate, conv_mix, conv_input, conv_taps):
    gated_in = (conv_mix.astype(f32) * conv_input.astype(f32)).astype(bf16)
    extended = jnp.concatenate([before, gated_in], axis=0).astype(f32)
    taps = conv_taps.astype(f32)
    convolved = taps[0] * extended[:-2] + taps[1] * extended[1:-1] + taps[2] * extended[2:]
    return (conv_gate.astype(f32) * convolved).astype(bf16)


def shards(
    conv_gate,
    conv_mix,
    conv_input,
    conv_taps,
    query_rows,
    key_rows,
    value_rows,
    lambdas,
    head_gain,
    w_out_conv,
    w_out_heads,
):
    rows = query_rows.shape[0]
    count = lax.axis_size("sp")
    lines = count // (PLANES * CORES)
    own = lax.axis_index("sp")
    in_plane = lines * CORES
    z = own // in_plane
    at = jnp.stack([z // 2, z % 2, own % in_plane // CORES, own % CORES]).astype(jnp.int32)

    def place(p, e, x, c):
        return ((2 * p + e) * lines + x) * CORES + c

    peers = [
        [place(p, e, x, c) for e in range(2) for x in range(lines)]
        for p in range(PLANES // 2)
        for c in range(CORES)
    ]
    column = [
        [place(p, e, x, c) for p in range(PLANES // 2) for c in range(CORES)]
        for e in range(2)
        for x in range(lines)
    ]
    ways = lax.axis_size("tp")
    peers_by_head = [[member * ways + y for member in group for y in range(ways)] for group in peers]
    early, late, copies = pack(query_rows, key_rows, value_rows, 2 * lines)
    late = lax.all_gather(late, "sp", axis=0, tiled=True, axis_index_groups=column)
    queries = lax.all_to_all(
        copies, "sp", split_axis=0, concat_axis=0, tiled=True, axis_index_groups=peers
    ).reshape(2 * lines * rows, -1)
    before = halo(conv_mix, conv_input)
    early = lax.all_gather(early, "sp", axis=0, tiled=True, axis_index_groups=column)
    early, before = lax.optimization_barrier((early, before))
    state = flash(at, queries, early, rows, 0, EARLY, ())
    w_heads, state = lax.optimization_barrier((w_out_heads, state))
    w_heads = lax.all_gather(w_heads, "tp", axis=0, tiled=True)
    parts = flash(at, queries, late, rows, EARLY, rows - EARLY, (lambdas, *state))
    parts, before = lax.optimization_barrier((parts, before))
    arrived = lax.all_to_all(
        parts.reshape(2 * lines * ways, OUT_ROWS, 128),
        ("sp", "tp"),
        split_axis=0,
        concat_axis=0,
        tiled=True,
        axis_index_groups=peers_by_head,
    ).reshape(2 * lines, ways, OUT_ROWS, 128)
    conv_out = conv_branch(before, conv_gate, conv_mix, conv_input, conv_taps)
    conv_part = jnp.dot(conv_out, w_out_conv, preferred_element_type=f32).astype(bf16)
    conv_part = conv_part.reshape(ways, rows // ways, -1)
    own_y = lax.axis_index("tp")
    conv_parts = []
    for k in range(ways):
        piece = lax.dynamic_index_in_dim(conv_part, (own_y + k) % ways, 0, keepdims=False)
        if k:
            piece = lax.ppermute(piece, "tp", [(y, (y + k) % ways) for y in range(ways)])
        conv_parts.append(piece)
    tp = lax.axis_index("tp").astype(jnp.int32)[None]
    return merge(tp, head_gain, arrived, w_heads, conv_parts)


def solution(mesh):
    placed = (
        P("sp", "tp"),
        P("sp", "tp"),
        P("sp", "tp"),
        P(None, "tp"),
        P("sp", "tp"),
        P("sp", "tp"),
        P("sp", "tp"),
        P("tp"),
        P(),
        P("tp", None),
        P("tp", None),
    )
    return jax.shard_map(
        shards, mesh=mesh, in_specs=placed, out_specs=P(("sp", "tp"), None), check_vma=False
    )
```

```python
import math

import jax
import jax.numpy as jnp
from jax import lax
from jax.experimental import pallas as pl
from jax.experimental.pallas import tpu as pltpu
from jax.sharding import PartitionSpec as P

f32, bf16 = jnp.float32, jnp.bfloat16
HEAD_QK = 64
HEAD_V = 128
MAPS = 2
PLANES = 16
CORES = 2
Q_STEP = 512
K_STEP = 256
SCALE = HEAD_QK**-0.5 * math.log2(math.e)
LOW = -1e30
MASKED = -2e30
STAT = 16
OUT_ROWS = HEAD_V + STAT
NN = (((1,), (0,)), ((), ()))


def pack_kernel(q_ref, k_ref, v_ref, pair_ref, copies_ref):
    pair_ref[:, :HEAD_V] = k_ref[...]
    pair_ref[:, HEAD_V:] = v_ref[...]
    for i in range(copies_ref.shape[0]):
        copies_ref[i] = q_ref[...]


def pack(q, k, v, copies):
    rows, width = q.shape
    return pl.pallas_call(
        pack_kernel,
        out_shape=[
            jax.ShapeDtypeStruct((rows, 2 * width), bf16),
            jax.ShapeDtypeStruct((copies, rows, width), bf16),
        ],
        name="pack",
    )(q, k, v)


def flash_kernel(rows, at, lam, q_ref, kv_hbm, out_hbm, *refs):
    kv_ref, out_ref, kv_sems, out_sems, m_s, acc, qt, s_a, s_b, b_a, b_b = refs
    head, tail = (
        pltpu.make_async_copy(kv_hbm.at[part], kv_ref.at[part], kv_sems.at[i])
        for i, part in enumerate((pl.ds(0, K_STEP), pl.ds(K_STEP, kv_ref.shape[0] - K_STEP)))
    )
    head.start()
    tail.start()
    shards = q_ref.shape[0] // rows
    blocks = q_ref.shape[0] // Q_STEP
    lines = shards // 2
    p, e, x, c = at[0], at[1], at[2], at[3]

    def prepare(i, _):
        blk = q_ref[pl.ds(i * rows, rows), :].astype(f32).T * SCALE
        high = blk.astype(bf16).astype(f32)
        rest = blk - high
        for m in range(MAPS):
            lo, hi = HEAD_QK * m, HEAD_QK * (m + 1)
            qt[m, :, pl.ds(i * rows, rows)] = jnp.zeros((4 * HEAD_QK, rows), bf16)
            qt[m, lo:hi, pl.ds(i * rows, rows)] = high[lo:hi].astype(bf16)
            qt[m, 128 + lo : 128 + hi, pl.ds(i * rows, rows)] = rest[lo:hi].astype(bf16)
        return 0

    lax.fori_loop(0, shards, prepare, 0)
    m_s[...] = jnp.full(m_s.shape, LOW, f32)
    acc[...] = jnp.zeros(acc.shape, f32)
    scores = ((s_a, b_a), (s_b, b_b))

    def cols(b):
        return slice(b * Q_STEP, (b + 1) * Q_STEP)

    def score(i, b, ahead):
        s_ref, b_ref = scores[b % 2]
        k = kv_ref[pl.ds(i * K_STEP, K_STEP), :HEAD_V]
        k = jnp.concatenate([k, k], axis=1)
        for m in range(MAPS):
            s = lax.dot_general(k, qt[m, :, cols(b)], NN, preferred_element_type=f32)
            if ahead is not None:
                parts = []
                for h in range(Q_STEP // rows):
                    g = b * (Q_STEP // rows) + h
                    first = ((g // lines) * shards + (g % lines) * CORES + c) * rows
                    parts.append(jnp.where(ahead <= first, s[:, h * rows : (h + 1) * rows], MASKED))
                s = jnp.concatenate(parts, axis=1)
            s_ref[m] = s
            b_ref[m] = jnp.max(s.reshape(K_STEP // 8, 8, Q_STEP), axis=0)

    def weigh(v, b):
        s_ref, b_ref = scores[b % 2]
        for m in range(MAPS):
            old = m_s[m, :, cols(b)]
            new = jnp.maximum(old, jnp.max(b_ref[m], axis=0, keepdims=True))
            weights = jnp.exp2(s_ref[m] - new[:1]).astype(bf16)
            shrink = jnp.exp2(old - new)
            m_s[m, :, cols(b)] = new
            o = lax.dot_general(v, weights, NN, preferred_element_type=f32)
            acc[m, :, cols(b)] = acc[m, :, cols(b)] * shrink[:1] + o

    def values(i):
        v = kv_ref[pl.ds(i * K_STEP, K_STEP), HEAD_V:].astype(f32).T.astype(bf16)
        return jnp.concatenate([v, jnp.ones((STAT, K_STEP), bf16)], axis=0)

    full = CORES * p
    head.wait()
    score(0, 0, None)
    tail.wait()

    def body(i, _):
        v = values(i)
        for b in range(blocks):
            if b + 1 < blocks:
                score(i, b + 1, None)
            else:
                score(i + 1, 0, None)
            weigh(v, b)
        return 0

    lax.fori_loop(0, full, body, 0)

    def edge(i, _):
        base = (e * shards + x * CORES + i - full) * rows
        ahead = (
            lax.broadcasted_iota(jnp.int32, (K_STEP, rows), 0)
            - lax.broadcasted_iota(jnp.int32, (K_STEP, rows), 1)
            + base
        )
        v = values(i)
        score(i, 0, ahead)
        for b in range(blocks):
            if b + 1 < blocks:
                score(i, b + 1, ahead)
            weigh(v, b)
        return 0

    lax.fori_loop(full, full + CORES, edge, 0)

    def leave(s):
        return pltpu.make_async_copy(out_ref.at[s], out_hbm.at[s], out_sems.at[s])

    def finish(s, _):
        at_cols = pl.ds(s * rows, rows)
        sides = []
        for m in range(MAPS):
            a = acc[m, :, at_cols]
            den = jnp.maximum(a[HEAD_V : HEAD_V + 8], 1e-30)
            factor = lam[0] / den[:1] if m else 1.0 / den[:1]
            rest = m_s[m, :, at_cols] + jnp.log2(den)
            parts = []
            for _part in range(3):
                hi = rest.astype(bf16).astype(f32)
                parts.append(hi)
                rest = rest - hi
            r = lax.broadcasted_iota(jnp.int32, rest.shape, 0)
            stat = jnp.where(r == 0, parts[0], jnp.where(r == 1, parts[1], parts[2]))
            sides.append(jnp.concatenate([a[:HEAD_V] * factor, stat, stat], axis=0))
        for t in range(rows // 128):
            first = sides[0][:, t * 128 : (t + 1) * 128]
            second = pltpu.roll(sides[1][:, t * 128 : (t + 1) * 128], 64, 1)
            lower = lax.broadcasted_iota(jnp.int32, first.shape, 1) < 64
            out_ref[s, 2 * t] = jnp.where(lower, first, second).astype(bf16)
            out_ref[s, 2 * t + 1] = jnp.where(lower, second, first).astype(bf16)
        leave(s).start()
        return 0

    lax.fori_loop(0, shards, finish, 0)
    for s in range(shards):
        leave(s).wait()


def flash(at, lambdas, q, kv, rows):
    queries = q.shape[0]
    shards = queries // rows
    out = (shards, rows // 64, OUT_ROWS, 128)
    hbm = pl.BlockSpec(memory_space=pl.ANY)
    smem = pl.BlockSpec(memory_space=pltpu.SMEM)

    def body(*refs):
        flash_kernel(rows, *refs)

    return pl.pallas_call(
        body,
        out_shape=jax.ShapeDtypeStruct(out, bf16),
        in_specs=[smem, smem, pl.BlockSpec(memory_space=pltpu.VMEM), hbm],
        out_specs=hbm,
        scratch_shapes=[
            pltpu.VMEM(kv.shape, bf16),
            pltpu.VMEM(out, bf16),
            pltpu.SemaphoreType.DMA((2,)),
            pltpu.SemaphoreType.DMA((shards,)),
            pltpu.VMEM((MAPS, 8, queries), f32),
            pltpu.VMEM((MAPS, HEAD_V + STAT, queries), f32),
            pltpu.VMEM((MAPS, 4 * HEAD_QK, queries), bf16),
            pltpu.VMEM((MAPS, K_STEP, Q_STEP), f32),
            pltpu.VMEM((MAPS, K_STEP, Q_STEP), f32),
            pltpu.VMEM((MAPS, 8, Q_STEP), f32),
            pltpu.VMEM((MAPS, 8, Q_STEP), f32),
        ],
        name="flash",
    )(at, lambdas, q, kv)


def merge_kernel(ways, tp, gain, *refs):
    sources, (out_ref, parts, conv, w), sems = refs[: 2 + ways], refs[2 + ways : -1], refs[-1]
    depth = w.shape[0] // ways
    held = [parts, conv] + [w.at[pl.ds(k * depth, depth)] for k in range(ways)]
    copies = [
        pltpu.make_async_copy(src, dst, sems.at[i])
        for i, (src, dst) in enumerate(zip(sources, held))
    ]
    for copy in copies:
        copy.start()
    copies[0].wait()
    count, _, _, lanes = parts.shape
    half = lanes // 2
    blocks = []
    for k in range(ways):
        h = (tp[0] + ways - k) % ways
        logs = []
        for d in range(count):
            stat = parts[d, h, HEAD_V:, :].astype(f32)
            logs.append(stat[0:1] + stat[1:2] + stat[2:3])
        peak = logs[0]
        for d in range(1, count):
            peak = jnp.maximum(peak, logs[d])
        weights = [jnp.exp2(x - peak) for x in logs]
        inverse = 1.0 / sum(weights)
        total = jnp.zeros((HEAD_V, lanes), f32)
        for d in range(count):
            total += parts[d, h, :HEAD_V, :].astype(f32) * (weights[d] * inverse)
        diff = total - pltpu.roll(total, half, 1)
        square = jnp.mean(diff * diff, axis=0, keepdims=True)
        heads = (diff * lax.rsqrt(square + 1e-6)).T * (gain[...] * 0.8)
        blocks.append(jnp.where(tp[0] % 2 == 1, heads[half:], heads[:half]).astype(bf16))
    heads = jnp.concatenate(blocks, axis=1)
    for copy in copies[1:]:
        copy.wait()
    out_ref[...] = (
        lax.dot_general(heads, w[...], NN, preferred_element_type=f32) + conv[...]
    ).astype(bf16)


def merge(tp, head_gain, parts, conv, weights):
    ways = len(weights)
    depth, width = weights[0].shape

    def body(*refs):
        merge_kernel(ways, *refs)

    return pl.pallas_call(
        body,
        out_shape=jax.ShapeDtypeStruct(conv.shape, bf16),
        in_specs=[pl.BlockSpec(memory_space=pltpu.SMEM), pl.BlockSpec(memory_space=pltpu.VMEM)]
        + [pl.BlockSpec(memory_space=pl.ANY)] * (2 + ways),
        out_specs=pl.BlockSpec(memory_space=pltpu.VMEM),
        scratch_shapes=[
            pltpu.VMEM(parts.shape, bf16),
            pltpu.VMEM(conv.shape, f32),
            pltpu.VMEM((ways * depth, width), bf16),
            pltpu.SemaphoreType.DMA((2 + ways,)),
        ],
        name="merge",
    )(tp, head_gain[None, :], parts, conv, *weights)


def halo(conv_mix, conv_input):
    count = lax.axis_size("sp")
    gated_in = (conv_mix.astype(f32) * conv_input.astype(f32)).astype(bf16)
    return lax.ppermute(gated_in[-2:], "sp", [(s, s + 1) for s in range(count - 1)])


def conv_branch(before, conv_gate, conv_mix, conv_input, conv_taps):
    gated_in = (conv_mix.astype(f32) * conv_input.astype(f32)).astype(bf16)
    extended = jnp.concatenate([before, gated_in], axis=0).astype(f32)
    taps = conv_taps.astype(f32)
    convolved = taps[0] * extended[:-2] + taps[1] * extended[1:-1] + taps[2] * extended[2:]
    return (conv_gate.astype(f32) * convolved).astype(bf16)


def shards(
    conv_gate,
    conv_mix,
    conv_input,
    conv_taps,
    query_rows,
    key_rows,
    value_rows,
    lambdas,
    head_gain,
    w_out_conv,
    w_out_heads,
):
    rows = query_rows.shape[0]
    count = lax.axis_size("sp")
    lines = count // (PLANES * CORES)
    own = lax.axis_index("sp")
    in_plane = lines * CORES
    z = own // in_plane
    at = jnp.stack([z // 2, z % 2, own % in_plane // CORES, own % CORES]).astype(jnp.int32)

    def place(p, e, x, c):
        return ((2 * p + e) * lines + x) * CORES + c

    peers = [
        [place(p, e, x, c) for e in range(2) for x in range(lines)]
        for p in range(PLANES // 2)
        for c in range(CORES)
    ]
    column = [
        [place(p, e, x, c) for p in range(PLANES // 2) for c in range(CORES)]
        for e in range(2)
        for x in range(lines)
    ]
    ways = lax.axis_size("tp")
    peers_by_head = [[member * ways + y for member in group for y in range(ways)] for group in peers]
    ways = lax.axis_size("tp")
    peers_by_head = [[member * ways + y for member in group for y in range(ways)] for group in peers]
    pair, copies = pack(query_rows, key_rows, value_rows, 2 * lines)
    keys = lax.all_gather(pair, "sp", axis=0, tiled=True, axis_index_groups=column)
    queries = lax.all_to_all(
        copies, "sp", split_axis=0, concat_axis=0, tiled=True, axis_index_groups=peers
    ).reshape(2 * lines * rows, -1)

    def moved(value, k):
        return lax.ppermute(value, "tp", [(y, (y + k) % ways) for y in range(ways)])

    before = halo(conv_mix, conv_input)
    weights = [w_out_heads] + [moved(w_out_heads, k) for k in range(1, ways - 1)]
    last_source, queries = lax.optimization_barrier((w_out_heads, queries))
    weights.append(moved(last_source, ways - 1))
    conv_out = conv_branch(before, conv_gate, conv_mix, conv_input, conv_taps)
    conv_part = jnp.dot(conv_out, w_out_conv, preferred_element_type=f32).astype(bf16)
    conv_part = conv_part.reshape(ways, rows // ways, -1)
    own_y = lax.axis_index("tp")
    conv_sum = jnp.zeros(conv_part.shape[1:], f32)
    for k in range(ways):
        piece = lax.dynamic_index_in_dim(conv_part, (own_y + k) % ways, 0, keepdims=False)
        conv_sum += (moved(piece, k) if k else piece).astype(f32)
    keys, weights, conv_sum = lax.optimization_barrier((keys, weights, conv_sum))
    parts = flash(at, lambdas, queries, keys, rows)
    arrived = lax.all_to_all(
        parts.reshape(2 * lines * ways, OUT_ROWS, 128),
        ("sp", "tp"),
        split_axis=0,
        concat_axis=0,
        tiled=True,
        axis_index_groups=peers_by_head,
    ).reshape(2 * lines, ways, OUT_ROWS, 128)
    return merge(own_y.astype(jnp.int32)[None], head_gain, arrived, conv_sum, weights)


def solution(mesh):
    placed = (
        P("sp", "tp"),
        P("sp", "tp"),
        P("sp", "tp"),
        P(None, "tp"),
        P("sp", "tp"),
        P("sp", "tp"),
        P("sp", "tp"),
        P("tp"),
        P(),
        P("tp", None),
        P("tp", None),
    )
    return jax.shard_map(
        shards, mesh=mesh, in_specs=placed, out_specs=P(("sp", "tp"), None), check_vma=False
    )
```

```python
import math

import jax
import jax.numpy as jnp
from jax import lax
from jax.experimental import pallas as pl
from jax.experimental.pallas import tpu as pltpu
from jax.sharding import PartitionSpec as P


f32, bf16 = jnp.float32, jnp.bfloat16
HEAD_QK = 64
HEAD_V = 128
MAPS = 2
PLANES = 16
CORES = 2
Q_STEP = 256
K_STEP = 512
SCALE = HEAD_QK**-0.5 * math.log2(math.e)
LOW = -1e30
MASKED = -2e30
STAT = 16
OUT_ROWS = HEAD_V + 8
NN = (((1,), (0,)), ((), ()))


def pack_kernel(q_ref, k_ref, v_ref, pair_ref, copies_ref):
    pair_ref[:, :HEAD_V] = k_ref[...]
    pair_ref[:, HEAD_V:] = v_ref[...]
    for i in range(copies_ref.shape[0]):
        copies_ref[i] = q_ref[...]


def pack(q, k, v, copies):
    rows, width = q.shape
    return pl.pallas_call(
        pack_kernel,
        out_shape=[
            jax.ShapeDtypeStruct((rows, 2 * width), bf16),
            jax.ShapeDtypeStruct((copies, rows, width), bf16),
        ],
        name="pack",
    )(q, k, v)


def flash_kernel(rows, at, lam, q_ref, kv_hbm, out_hbm, *refs):
    kv_ref, out_ref, kv_sems, out_sems, m_s, acc, qt, s_a, s_b, b_a, b_b = refs
    full = at[0]
    end = full + 1

    def come(i):
        part = pl.ds(i * K_STEP, K_STEP)
        return pltpu.make_async_copy(kv_hbm.at[part], kv_ref.at[part], kv_sems.at[i])

    def fetch(i, _):
        come(i).start()
        return 0

    lax.fori_loop(0, end, fetch, 0)
    shards = q_ref.shape[0] // rows
    blocks = q_ref.shape[0] // Q_STEP
    lines = shards // 2
    e, x, c = at[1], at[2], at[3]

    def prepare(i, _):
        blk = q_ref[pl.ds(i * rows, rows), :].astype(f32).T * SCALE
        high = blk.astype(bf16).astype(f32)
        rest = blk - high
        for m in range(MAPS):
            lo, hi = HEAD_QK * m, HEAD_QK * (m + 1)
            qt[m, :, pl.ds(i * rows, rows)] = jnp.zeros((4 * HEAD_QK, rows), bf16)
            qt[m, lo:hi, pl.ds(i * rows, rows)] = high[lo:hi].astype(bf16)
            qt[m, 128 + lo : 128 + hi, pl.ds(i * rows, rows)] = rest[lo:hi].astype(bf16)
        return 0

    lax.fori_loop(0, shards, prepare, 0)
    m_s[...] = jnp.full(m_s.shape, LOW, f32)
    acc[...] = jnp.zeros(acc.shape, f32)
    scores = ((s_a, b_a), (s_b, b_b))

    def cols(b):
        return slice(b * Q_STEP, (b + 1) * Q_STEP)

    def score(i, b, ahead):
        s_ref, b_ref = scores[b % 2]
        k = kv_ref[pl.ds(i * K_STEP, K_STEP), :HEAD_V]
        k = jnp.concatenate([k, k], axis=1)
        for m in range(MAPS):
            s = lax.dot_general(k, qt[m, :, cols(b)], NN, preferred_element_type=f32)
            if ahead is not None:
                parts = []
                for h in range(Q_STEP // rows):
                    g = b * (Q_STEP // rows) + h
                    first = ((g // lines) * shards + (g % lines) * CORES + c) * rows
                    parts.append(jnp.where(ahead <= first, s[:, h * rows : (h + 1) * rows], MASKED))
                s = jnp.concatenate(parts, axis=1)
            s_ref[m] = s
            b_ref[m] = jnp.max(s.reshape(K_STEP // 8, 8, Q_STEP), axis=0)

    def weigh(v, b):
        s_ref, b_ref = scores[b % 2]
        for m in range(MAPS):
            old = m_s[m, :, cols(b)]
            new = jnp.maximum(old, jnp.max(b_ref[m], axis=0, keepdims=True))
            weights = jnp.exp2(s_ref[m] - new[:1]).astype(bf16)
            shrink = jnp.exp2(old - new)
            m_s[m, :, cols(b)] = new
            o = lax.dot_general(v, weights, NN, preferred_element_type=f32)
            acc[m, :, cols(b)] = acc[m, :, cols(b)] * shrink[:1] + o

    def values(i):
        v = kv_ref[pl.ds(i * K_STEP, K_STEP), HEAD_V:].astype(f32).T.astype(bf16)
        return jnp.concatenate([v, jnp.ones((STAT, K_STEP), bf16)], axis=0)

    come(0).wait()
    score(0, 0, None)

    def body(i, _):
        come(i + 1).wait()
        v = values(i)
        for b in range(blocks):
            if b + 1 < blocks:
                score(i, b + 1, None)
            else:
                score(i + 1, 0, None)
            weigh(v, b)
        return 0

    lax.fori_loop(0, full, body, 0)

    def edge(i, _):
        base = (e * shards + x * CORES) * rows
        ahead = (
            lax.broadcasted_iota(jnp.int32, (K_STEP, rows), 0)
            - lax.broadcasted_iota(jnp.int32, (K_STEP, rows), 1)
            + base
        )
        v = values(i)
        score(i, 0, ahead)
        for b in range(blocks):
            if b + 1 < blocks:
                score(i, b + 1, ahead)
            weigh(v, b)
        return 0

    lax.fori_loop(full, end, edge, 0)

    def leave(s):
        return pltpu.make_async_copy(out_ref.at[s], out_hbm.at[s], out_sems.at[s])

    def finish(s, _):
        at_cols = pl.ds(s * rows, rows)
        sides = []
        for m in range(MAPS):
            a = acc[m, :, at_cols]
            den = jnp.maximum(a[HEAD_V : HEAD_V + 8], 1e-30)
            factor = lam[0] / den[:1] if m else 1.0 / den[:1]
            rest = m_s[m, :, at_cols] + jnp.log2(den)
            parts = []
            for _ in range(3):
                hi = rest.astype(bf16).astype(f32)
                parts.append(hi)
                rest = rest - hi
            r = lax.broadcasted_iota(jnp.int32, rest.shape, 0)
            stat = jnp.where(r == 0, parts[0], jnp.where(r == 1, parts[1], parts[2]))
            sides.append(jnp.concatenate([a[:HEAD_V] * factor, stat], axis=0))
        for t in range(rows // 128):
            first = sides[0][:, t * 128 : (t + 1) * 128]
            second = pltpu.roll(sides[1][:, t * 128 : (t + 1) * 128], 64, 1)
            lower = lax.broadcasted_iota(jnp.int32, first.shape, 1) < 64
            out_ref[s, 2 * t] = jnp.where(lower, first, second).astype(bf16)
            out_ref[s, 2 * t + 1] = jnp.where(lower, second, first).astype(bf16)
        leave(s).start()
        return 0

    lax.fori_loop(0, shards, finish, 0)
    for s in range(shards):
        leave(s).wait()


def flash(at, lambdas, q, kv, rows):
    queries = q.shape[0]
    shards = queries // rows
    out = (shards, rows // 64, OUT_ROWS, 128)
    hbm = pl.BlockSpec(memory_space=pl.ANY)
    smem = pl.BlockSpec(memory_space=pltpu.SMEM)

    def body(*refs):
        flash_kernel(rows, *refs)

    return pl.pallas_call(
        body,
        out_shape=jax.ShapeDtypeStruct(out, bf16),
        in_specs=[smem, smem, pl.BlockSpec(memory_space=pltpu.VMEM), hbm],
        out_specs=hbm,
        scratch_shapes=[
            pltpu.VMEM(kv.shape, bf16),
            pltpu.VMEM(out, bf16),
            pltpu.SemaphoreType.DMA((kv.shape[0] // K_STEP,)),
            pltpu.SemaphoreType.DMA((shards,)),
            pltpu.VMEM((MAPS, 8, queries), f32),
            pltpu.VMEM((MAPS, HEAD_V + STAT, queries), f32),
            pltpu.VMEM((MAPS, 4 * HEAD_QK, queries), bf16),
            pltpu.VMEM((MAPS, K_STEP, Q_STEP), f32),
            pltpu.VMEM((MAPS, K_STEP, Q_STEP), f32),
            pltpu.VMEM((MAPS, 8, Q_STEP), f32),
            pltpu.VMEM((MAPS, 8, Q_STEP), f32),
        ],
        name="flash",
    )(at, lambdas, q, kv)


def merge_kernel(ways, tp, gain, *refs):
    sources, (out_ref, parts, conv, w), sems = refs[: 2 + ways], refs[2 + ways : -1], refs[-1]
    depth = w.shape[0] // ways
    held = [parts, conv] + [w.at[pl.ds(k * depth, depth)] for k in range(ways)]
    copies = [
        pltpu.make_async_copy(src, dst, sems.at[i])
        for i, (src, dst) in enumerate(zip(sources, held))
    ]
    for copy in copies:
        copy.start()
    copies[0].wait()
    count, _, _, lanes = parts.shape
    half = lanes // 2
    blocks = []
    for k in range(ways):
        h = (tp[0] + ways - k) % ways
        logs = []
        for d in range(count):
            stat = parts[d, h, HEAD_V:, :].astype(f32)
            logs.append(stat[0:1] + stat[1:2] + stat[2:3])
        peak = logs[0]
        for d in range(1, count):
            peak = jnp.maximum(peak, logs[d])
        weights = [jnp.exp2(x - peak) for x in logs]
        inverse = 1.0 / sum(weights)
        total = jnp.zeros((HEAD_V, lanes), f32)
        for d in range(count):
            total += parts[d, h, :HEAD_V, :].astype(f32) * (weights[d] * inverse)
        diff = total - pltpu.roll(total, half, 1)
        square = jnp.mean(diff * diff, axis=0, keepdims=True)
        heads = (diff * lax.rsqrt(square + 1e-6)).T * (gain[...] * 0.8)
        blocks.append(jnp.where(tp[0] % 2 == 1, heads[half:], heads[:half]).astype(bf16))
    heads = jnp.concatenate(blocks, axis=1)
    for copy in copies[1:]:
        copy.wait()
    out_ref[...] = (
        lax.dot_general(heads, w[...], NN, preferred_element_type=f32) + conv[...]
    ).astype(bf16)


def merge(tp, head_gain, parts, conv, weights):
    ways = len(weights)
    depth, width = weights[0].shape

    def body(*refs):
        merge_kernel(ways, *refs)

    return pl.pallas_call(
        body,
        out_shape=jax.ShapeDtypeStruct(conv.shape, bf16),
        in_specs=[pl.BlockSpec(memory_space=pltpu.SMEM), pl.BlockSpec(memory_space=pltpu.VMEM)]
        + [pl.BlockSpec(memory_space=pl.ANY)] * (2 + ways),
        out_specs=pl.BlockSpec(memory_space=pltpu.VMEM),
        scratch_shapes=[
            pltpu.VMEM(parts.shape, bf16),
            pltpu.VMEM(conv.shape, f32),
            pltpu.VMEM((ways * depth, width), bf16),
            pltpu.SemaphoreType.DMA((2 + ways,)),
        ],
        name="merge",
    )(tp, head_gain[None, :], parts, conv, *weights)


def halo(conv_mix, conv_input):
    count = lax.axis_size("sp")
    gated_in = (conv_mix.astype(f32) * conv_input.astype(f32)).astype(bf16)
    return lax.ppermute(gated_in[-2:], "sp", [(s, s + 1) for s in range(count - 1)])


def conv_branch(before, conv_gate, conv_mix, conv_input, conv_taps):
    gated_in = (conv_mix.astype(f32) * conv_input.astype(f32)).astype(bf16)
    extended = jnp.concatenate([before, gated_in], axis=0).astype(f32)
    taps = conv_taps.astype(f32)
    convolved = taps[0] * extended[:-2] + taps[1] * extended[1:-1] + taps[2] * extended[2:]
    return (conv_gate.astype(f32) * convolved).astype(bf16)


def layer(
    conv_gate,
    conv_mix,
    conv_input,
    conv_taps,
    query_rows,
    key_rows,
    value_rows,
    lambdas,
    head_gain,
    w_out_conv,
    w_out_heads,
):
    rows = query_rows.shape[0]
    count = lax.axis_size("sp")
    lines = count // (PLANES * CORES)
    own = lax.axis_index("sp")
    in_plane = lines * CORES
    z = own // in_plane
    at = jnp.stack([z // 2, z % 2, own % in_plane // CORES, own % CORES]).astype(jnp.int32)

    def place(p, e, x, c):
        return ((2 * p + e) * lines + x) * CORES + c

    peers = [
        [place(p, e, x, c) for e in range(2) for x in range(lines)]
        for p in range(PLANES // 2)
        for c in range(CORES)
    ]
    column = [
        [place(p, e, x, c) for p in range(PLANES // 2) for c in range(CORES)]
        for e in range(2)
        for x in range(lines)
    ]
    ways = lax.axis_size("tp")
    peers_by_head = [[member * ways + y for member in group for y in range(ways)] for group in peers]
    ways = lax.axis_size("tp")
    peers_by_head = [[member * ways + y for member in group for y in range(ways)] for group in peers]
    pair, copies = pack(query_rows, key_rows, value_rows, 2 * lines)
    keys = lax.all_gather(pair, "sp", axis=0, tiled=True, axis_index_groups=column)
    queries = lax.all_to_all(
        copies, "sp", split_axis=0, concat_axis=0, tiled=True, axis_index_groups=peers
    ).reshape(2 * lines * rows, -1)

    def moved(value, k):
        return lax.ppermute(value, "tp", [(y, (y + k) % ways) for y in range(ways)])

    before = halo(conv_mix, conv_input)
    weights = [w_out_heads]
    for k in range(1, ways):
        weights.append(moved(w_out_heads, k))
    conv_out = conv_branch(before, conv_gate, conv_mix, conv_input, conv_taps)
    conv_part = jnp.dot(conv_out, w_out_conv, preferred_element_type=f32).astype(bf16)
    conv_part = conv_part.reshape(ways, rows // ways, -1)
    own_y = lax.axis_index("tp")
    conv_sum = jnp.zeros(conv_part.shape[1:], f32)
    for k in range(ways):
        piece = lax.dynamic_index_in_dim(conv_part, (own_y + k) % ways, 0, keepdims=False)
        if k == ways - 1:
            piece, queries = lax.optimization_barrier((piece, queries))
        if k:
            piece = moved(piece, k)
        conv_sum += piece.astype(f32)
    keys, weights, conv_sum = lax.optimization_barrier((keys, weights, conv_sum))
    parts = flash(at, lambdas, queries, keys, rows)
    arrived = lax.all_to_all(
        parts.reshape(2 * lines * ways, OUT_ROWS, 128),
        ("sp", "tp"),
        split_axis=0,
        concat_axis=0,
        tiled=True,
        axis_index_groups=peers_by_head,
    ).reshape(2 * lines, ways, OUT_ROWS, 128)
    return merge(own_y.astype(jnp.int32)[None], head_gain, arrived, conv_sum, weights)


def solution(mesh):
    placed = (
        P("sp", "tp"),
        P("sp", "tp"),
        P("sp", "tp"),
        P(None, "tp"),
        P("sp", "tp"),
        P("sp", "tp"),
        P("sp", "tp"),
        P("tp"),
        P(),
        P("tp", None),
        P("tp", None),
    )
    return jax.shard_map(
        layer, mesh=mesh, in_specs=placed, out_specs=P(("sp", "tp"), None), check_vma=False
    )
```

```python
import math

import jax
import jax.numpy as jnp
from jax import lax
from jax.experimental import pallas as pl
from jax.experimental.pallas import tpu as pltpu
from jax.sharding import PartitionSpec as P


f32, bf16 = jnp.float32, jnp.bfloat16
HEAD_QK = 64
HEAD_V = 128
MAPS = 2
PLANES = 16
CORES = 2
Q_STEP = 256
K_STEP = 512
SCALE = HEAD_QK**-0.5 * math.log2(math.e)
LOW = -1e30
MASKED = -2e30
STAT = 16
OUT_ROWS = HEAD_V + 8
NN = (((1,), (0,)), ((), ()))


def pack_kernel(q_ref, k_ref, v_ref, pair_ref, copies_ref):
    pair_ref[:, :HEAD_V] = k_ref[...]
    pair_ref[:, HEAD_V:] = v_ref[...]
    for i in range(copies_ref.shape[0]):
        copies_ref[i] = q_ref[...]


def pack(q, k, v, copies):
    rows, width = q.shape
    return pl.pallas_call(
        pack_kernel,
        out_shape=[
            jax.ShapeDtypeStruct((rows, 2 * width), bf16),
            jax.ShapeDtypeStruct((copies, rows, width), bf16),
        ],
        name="pack",
    )(q, k, v)


def flash_kernel(rows, at, lam, q_ref, kv_hbm, out_hbm, *refs):
    kv_ref, out_ref, kv_sems, out_sems, m_s, acc, qt, s_a, s_b, b_a, b_b = refs
    full = at[0]
    end = full + 1

    def come(i):
        part = pl.ds(i * K_STEP, K_STEP)
        return pltpu.make_async_copy(kv_hbm.at[part], kv_ref.at[part], kv_sems.at[i])

    def fetch(i, _):
        come(i).start()
        return 0

    lax.fori_loop(0, end, fetch, 0)
    shards = q_ref.shape[0] // rows
    blocks = q_ref.shape[0] // Q_STEP
    lines = shards // 2
    e, x, c = at[1], at[2], at[3]

    def prepare(i, _):
        blk = q_ref[pl.ds(i * rows, rows), :].astype(f32).T * SCALE
        high = blk.astype(bf16).astype(f32)
        rest = blk - high
        for m in range(MAPS):
            lo, hi = HEAD_QK * m, HEAD_QK * (m + 1)
            qt[m, :, pl.ds(i * rows, rows)] = jnp.zeros((4 * HEAD_QK, rows), bf16)
            qt[m, lo:hi, pl.ds(i * rows, rows)] = high[lo:hi].astype(bf16)
            qt[m, 128 + lo : 128 + hi, pl.ds(i * rows, rows)] = rest[lo:hi].astype(bf16)
        return 0

    lax.fori_loop(0, shards, prepare, 0)
    m_s[...] = jnp.full(m_s.shape, LOW, f32)
    acc[...] = jnp.zeros(acc.shape, f32)
    scores = ((s_a, b_a), (s_b, b_b))

    def cols(b):
        return slice(b * Q_STEP, (b + 1) * Q_STEP)

    def score(i, b, ahead):
        s_ref, b_ref = scores[b % 2]
        k = kv_ref[pl.ds(i * K_STEP, K_STEP), :HEAD_V]
        k = jnp.concatenate([k, k], axis=1)
        for m in range(MAPS):
            s = lax.dot_general(k, qt[m, :, cols(b)], NN, preferred_element_type=f32)
            if ahead is not None:
                parts = []
                for h in range(Q_STEP // rows):
                    g = b * (Q_STEP // rows) + h
                    first = ((g // lines) * shards + (g % lines) * CORES + c) * rows
                    parts.append(jnp.where(ahead <= first, s[:, h * rows : (h + 1) * rows], MASKED))
                s = jnp.concatenate(parts, axis=1)
            s_ref[m] = s
            b_ref[m] = jnp.max(s.reshape(K_STEP // 8, 8, Q_STEP), axis=0)

    def weigh(v, b):
        s_ref, b_ref = scores[b % 2]
        for m in range(MAPS):
            old = m_s[m, :, cols(b)]
            new = jnp.maximum(old, jnp.max(b_ref[m], axis=0, keepdims=True))
            weights = jnp.exp2(s_ref[m] - new[:1]).astype(bf16)
            shrink = jnp.exp2(old - new)
            m_s[m, :, cols(b)] = new
            o = lax.dot_general(v, weights, NN, preferred_element_type=f32)
            acc[m, :, cols(b)] = acc[m, :, cols(b)] * shrink[:1] + o

    def values(i):
        v = kv_ref[pl.ds(i * K_STEP, K_STEP), HEAD_V:].astype(f32).T.astype(bf16)
        return jnp.concatenate([v, jnp.ones((STAT, K_STEP), bf16)], axis=0)

    come(0).wait()
    score(0, 0, None)

    def body(i, _):
        come(i + 1).wait()
        v = values(i)
        for b in range(blocks):
            if b + 1 < blocks:
                score(i, b + 1, None)
            else:
                score(i + 1, 0, None)
            weigh(v, b)
        return 0

    lax.fori_loop(0, full, body, 0)

    def edge(i, _):
        base = (e * shards + x * CORES) * rows
        ahead = (
            lax.broadcasted_iota(jnp.int32, (K_STEP, rows), 0)
            - lax.broadcasted_iota(jnp.int32, (K_STEP, rows), 1)
            + base
        )
        v = values(i)
        score(i, 0, ahead)
        for b in range(blocks):
            if b + 1 < blocks:
                score(i, b + 1, ahead)
            weigh(v, b)
        return 0

    lax.fori_loop(full, end, edge, 0)

    def leave(s):
        return pltpu.make_async_copy(out_ref.at[s], out_hbm.at[s], out_sems.at[s])

    def finish(s, _):
        at_cols = pl.ds(s * rows, rows)
        sides = []
        for m in range(MAPS):
            a = acc[m, :, at_cols]
            den = jnp.maximum(a[HEAD_V : HEAD_V + 8], 1e-30)
            factor = lam[0] / den[:1] if m else 1.0 / den[:1]
            rest = m_s[m, :, at_cols] + jnp.log2(den)
            parts = []
            for _ in range(3):
                hi = rest.astype(bf16).astype(f32)
                parts.append(hi)
                rest = rest - hi
            r = lax.broadcasted_iota(jnp.int32, rest.shape, 0)
            stat = jnp.where(r == 0, parts[0], jnp.where(r == 1, parts[1], parts[2]))
            sides.append(jnp.concatenate([a[:HEAD_V] * factor, stat], axis=0))
        for t in range(rows // 128):
            first = sides[0][:, t * 128 : (t + 1) * 128]
            second = pltpu.roll(sides[1][:, t * 128 : (t + 1) * 128], 64, 1)
            lower = lax.broadcasted_iota(jnp.int32, first.shape, 1) < 64
            out_ref[s, 2 * t] = jnp.where(lower, first, second).astype(bf16)
            out_ref[s, 2 * t + 1] = jnp.where(lower, second, first).astype(bf16)
        leave(s).start()
        return 0

    lax.fori_loop(0, shards, finish, 0)
    for s in range(shards):
        leave(s).wait()


def flash(at, lambdas, q, kv, rows):
    queries = q.shape[0]
    shards = queries // rows
    out = (shards, rows // 64, OUT_ROWS, 128)
    hbm = pl.BlockSpec(memory_space=pl.ANY)
    smem = pl.BlockSpec(memory_space=pltpu.SMEM)

    def body(*refs):
        flash_kernel(rows, *refs)

    return pl.pallas_call(
        body,
        out_shape=jax.ShapeDtypeStruct(out, bf16),
        in_specs=[smem, smem, pl.BlockSpec(memory_space=pltpu.VMEM), hbm],
        out_specs=hbm,
        scratch_shapes=[
            pltpu.VMEM(kv.shape, bf16),
            pltpu.VMEM(out, bf16),
            pltpu.SemaphoreType.DMA((kv.shape[0] // K_STEP,)),
            pltpu.SemaphoreType.DMA((shards,)),
            pltpu.VMEM((MAPS, 8, queries), f32),
            pltpu.VMEM((MAPS, HEAD_V + STAT, queries), f32),
            pltpu.VMEM((MAPS, 4 * HEAD_QK, queries), bf16),
            pltpu.VMEM((MAPS, K_STEP, Q_STEP), f32),
            pltpu.VMEM((MAPS, K_STEP, Q_STEP), f32),
            pltpu.VMEM((MAPS, 8, Q_STEP), f32),
            pltpu.VMEM((MAPS, 8, Q_STEP), f32),
        ],
        name="flash",
    )(at, lambdas, q, kv)


def merge_kernel(ways, tp, gain, *refs):
    sources, (out_ref, parts, conv, w), sems = refs[: 2 + ways], refs[2 + ways : -1], refs[-1]
    depth = w.shape[0] // ways
    held = [parts, conv] + [w.at[pl.ds(k * depth, depth)] for k in range(ways)]
    copies = [
        pltpu.make_async_copy(src, dst, sems.at[i])
        for i, (src, dst) in enumerate(zip(sources, held))
    ]
    for copy in copies:
        copy.start()
    copies[0].wait()
    count, _, _, lanes = parts.shape
    half = lanes // 2
    blocks = []
    for k in range(ways):
        h = (tp[0] + ways - k) % ways
        logs = []
        for d in range(count):
            stat = parts[d, h, HEAD_V:, :].astype(f32)
            logs.append(stat[0:1] + stat[1:2] + stat[2:3])
        peak = logs[0]
        for d in range(1, count):
            peak = jnp.maximum(peak, logs[d])
        weights = [jnp.exp2(x - peak) for x in logs]
        inverse = 1.0 / sum(weights)
        total = jnp.zeros((HEAD_V, lanes), f32)
        for d in range(count):
            total += parts[d, h, :HEAD_V, :].astype(f32) * (weights[d] * inverse)
        diff = total - pltpu.roll(total, half, 1)
        square = jnp.mean(diff * diff, axis=0, keepdims=True)
        heads = (diff * lax.rsqrt(square + 1e-6)).T * (gain[...] * 0.8)
        blocks.append(jnp.where(tp[0] % 2 == 1, heads[half:], heads[:half]).astype(bf16))
    heads = jnp.concatenate(blocks, axis=1)
    for copy in copies[1:]:
        copy.wait()
    out_ref[...] = (
        lax.dot_general(heads, w[...], NN, preferred_element_type=f32) + conv[...]
    ).astype(bf16)


def merge(tp, head_gain, parts, conv, weights):
    ways = len(weights)
    depth, width = weights[0].shape

    def body(*refs):
        merge_kernel(ways, *refs)

    return pl.pallas_call(
        body,
        out_shape=jax.ShapeDtypeStruct(conv.shape, bf16),
        in_specs=[pl.BlockSpec(memory_space=pltpu.SMEM), pl.BlockSpec(memory_space=pltpu.VMEM)]
        + [pl.BlockSpec(memory_space=pl.ANY)] * (2 + ways),
        out_specs=pl.BlockSpec(memory_space=pltpu.VMEM),
        scratch_shapes=[
            pltpu.VMEM(parts.shape, bf16),
            pltpu.VMEM(conv.shape, f32),
            pltpu.VMEM((ways * depth, width), bf16),
            pltpu.SemaphoreType.DMA((2 + ways,)),
        ],
        name="merge",
    )(tp, head_gain[None, :], parts, conv, *weights)


def halo(conv_mix, conv_input):
    count = lax.axis_size("sp")
    gated_in = (conv_mix.astype(f32) * conv_input.astype(f32)).astype(bf16)
    return lax.ppermute(gated_in[-2:], "sp", [(s, s + 1) for s in range(count - 1)])


def conv_branch(before, conv_gate, conv_mix, conv_input, conv_taps):
    gated_in = (conv_mix.astype(f32) * conv_input.astype(f32)).astype(bf16)
    extended = jnp.concatenate([before, gated_in], axis=0).astype(f32)
    taps = conv_taps.astype(f32)
    convolved = taps[0] * extended[:-2] + taps[1] * extended[1:-1] + taps[2] * extended[2:]
    return (conv_gate.astype(f32) * convolved).astype(bf16)


def layer(
    conv_gate,
    conv_mix,
    conv_input,
    conv_taps,
    query_rows,
    key_rows,
    value_rows,
    lambdas,
    head_gain,
    w_out_conv,
    w_out_heads,
):
    rows = query_rows.shape[0]
    count = lax.axis_size("sp")
    lines = count // (PLANES * CORES)
    own = lax.axis_index("sp")
    in_plane = lines * CORES
    z = own // in_plane
    at = jnp.stack([z // 2, z % 2, own % in_plane // CORES, own % CORES]).astype(jnp.int32)

    def place(p, e, x, c):
        return ((2 * p + e) * lines + x) * CORES + c

    peers = [
        [place(p, e, x, c) for e in range(2) for x in range(lines)]
        for p in range(PLANES // 2)
        for c in range(CORES)
    ]
    column = [
        [place(p, e, x, c) for p in range(PLANES // 2) for c in range(CORES)]
        for e in range(2)
        for x in range(lines)
    ]
    ways = lax.axis_size("tp")
    peers_by_head = [[member * ways + y for member in group for y in range(ways)] for group in peers]
    ways = lax.axis_size("tp")
    peers_by_head = [[member * ways + y for member in group for y in range(ways)] for group in peers]
    pair, copies = pack(query_rows, key_rows, value_rows, 2 * lines)
    keys = lax.all_gather(pair, "sp", axis=0, tiled=True, axis_index_groups=column)
    queries = lax.all_to_all(
        copies, "sp", split_axis=0, concat_axis=0, tiled=True, axis_index_groups=peers
    ).reshape(2 * lines * rows, -1)

    def moved(value, k):
        return lax.ppermute(value, "tp", [(y, (y + k) % ways) for y in range(ways)])

    before = halo(conv_mix, conv_input)
    weights = [w_out_heads]
    for k in range(1, ways):
        weights.append(moved(w_out_heads, k))
    conv_out = conv_branch(before, conv_gate, conv_mix, conv_input, conv_taps)
    conv_part = jnp.dot(conv_out, w_out_conv, preferred_element_type=f32).astype(bf16)
    conv_part = conv_part.reshape(ways, rows // ways, -1)
    own_y = lax.axis_index("tp")
    pieces = []
    for k in range(ways):
        piece = lax.dynamic_index_in_dim(conv_part, (own_y + k) % ways, 0, keepdims=False)
        if k == ways - 1:
            piece, queries = lax.optimization_barrier((piece, queries))
        if k:
            piece = moved(piece, k)
        pieces.append(piece)
    keys, weights, pieces = lax.optimization_barrier((keys, weights, pieces))
    parts = flash(at, lambdas, queries, keys, rows)
    parts, pieces = lax.optimization_barrier((parts, pieces))
    conv_sum = sum(piece.astype(f32) for piece in pieces)
    arrived = lax.all_to_all(
        parts.reshape(2 * lines * ways, OUT_ROWS, 128),
        ("sp", "tp"),
        split_axis=0,
        concat_axis=0,
        tiled=True,
        axis_index_groups=peers_by_head,
    ).reshape(2 * lines, ways, OUT_ROWS, 128)
    return merge(own_y.astype(jnp.int32)[None], head_gain, arrived, conv_sum, weights)


def solution(mesh):
    placed = (
        P("sp", "tp"),
        P("sp", "tp"),
        P("sp", "tp"),
        P(None, "tp"),
        P("sp", "tp"),
        P("sp", "tp"),
        P("sp", "tp"),
        P("tp"),
        P(),
        P("tp", None),
        P("tp", None),
    )
    return jax.shard_map(
        layer, mesh=mesh, in_specs=placed, out_specs=P(("sp", "tp"), None), check_vma=False
    )
```
